32 devices in a mesh: ep: 16 (over z, y, x), tp: 2 (over core).
Axes of the slice: x: 2, y: 2, z: 4, core: 2. Of those that a mesh axis runs over, the one named last changes fastest.
Arguments:
- tokens: bfloat16 [256, 2048], P('ep'), may hold values from -6 to 6
- norm_gain: float32 [2048], replicated, may hold values from 0.1 to 1.9
- query_weight: bfloat16 [2048, 1024], P('ep', 'tp'), may hold values from -0.125 to 0.125
- key_weight: bfloat16 [2048, 1024], P('ep', 'tp'), may hold values from -0.125 to 0.125
- value_weight: bfloat16 [2048, 1024], P('ep', 'tp'), may hold values from -0.125 to 0.125
- outgate_weight: bfloat16 [2048, 1024], P('ep', 'tp'), may hold values from -0.125 to 0.125
- input_weight: bfloat16 [2048, 8], P('ep', 'tp'), may hold values from -0.125 to 0.125
- forget_weight: bfloat16 [2048, 8], P('ep', 'tp'), may hold values from -0.125 to 0.125
- forget_bias: float32 [8], P('tp'), may hold values from -1 to 5
- memory: float32 [256, 8, 128, 128], P('ep', 'tp'), may hold values from -2.4 to 2.4
- stabilizer: float32 [256, 8], P('ep', 'tp'), may hold values from -3 to 3
- head_gain: float32 [1024], P('tp'), may hold values from 0.1 to 1.9
- mix_weight: bfloat16 [1024, 2048], P('tp', 'ep'), may hold values from -0.1875 to 0.1875
- second_gain: float32 [2048], replicated, may hold values from 0.1 to 1.9
- route_experts: int32 [256, 4], P('ep'), may hold values from 0 to 15, all different within a row; in each aligned block of 16 rows (0 to 15, 16 to 31, ...) at most 8 rows name the same one
- route_weight: float32 [256, 4], P('ep'), may hold values from 0.1 to 1
- expert_gate: bfloat16 [16, 2048, 2048], P('ep', None, 'tp'), may hold values from -0.5 to 0.5
- expert_up: bfloat16 [16, 2048, 2048], P('ep', None, 'tp'), may hold values from -0.5 to 0.5
- expert_down: bfloat16 [16, 2048, 2048], P('ep', 'tp'), may hold values from -0.03125 to 0.03125
- dense_gate: bfloat16 [4096, 2048], P(('ep', 'tp')), may hold values from -0.125 to 0.125
- dense_up: bfloat16 [4096, 2048], P(('ep', 'tp')), may hold values from -0.125 to 0.125
- dense_down: bfloat16 [4096, 2048], P(('ep', 'tp')), may hold values from -0.09375 to 0.09375
- branch_scale: float32 [2048], replicated, may hold values from 0.3 to 1.5
Outputs:
- mixed: bfloat16 [256, 2048], P('ep', 'tp')
- memory_new: float32 [256, 8, 128, 128], P('ep', 'tp')
- stabilizer_new: float32 [256, 8], P('ep', 'tp')
The draws below stay inside these ranges and needn't reach their ends.
Inputs may be any that keep to these rules, and one draw needn't show every extreme that they name: `route_experts`: each row names 4 different experts. Within each aligned block of 16 rows no expert is named by more than 8 rows, and in every draw some expert is named by exactly 8 rows of some block.
All inputs are finite; a program needn't handle non-finite values.
Results may differ from the reference program's by a relative error of at most 0.03.
Values may be sent and summed in bfloat16 or wider, within the bound.
A program may use at most 128 MiB of HBM per device.

```python
import math
import jax
import jax.numpy as jnp
import numpy as np
from jax import lax

MODEL = 2048
HEADS = 8
HEAD_SIZE = 128
HIDDEN_SIZE = 2048
DENSE = 4096
TOPK = 4
SEQ_GROUP = 16
BATCH = 256
EXPERTS = 16
CAPACITY = 8
N_EP = 16
N_TP = 2


def shard_levels(key, dims, shards, least, largest):
    def one(position, parts):
        steps = jax.random.uniform(jax.random.fold_in(jax.random.fold_in(key, 6), position), (parts,), jnp.float32, least / len(shards), largest / len(shards))
        return jnp.repeat(jnp.exp(steps), dims[position] // parts).reshape((-1,) + (1,) * (len(dims) - position - 1))

    level = one(*shards[0])
    for cut in shards[1:]:
        level = level * one(*cut)
    return level


def routed_block(rng, own, number, rows, count, top, most, lean):
    ranking = jax.random.permutation(rng, count)
    crowded, common = portions_of(count, rows * top, most, lean, True), portions_of(count, rows * top, most, lean, False)
    places = jnp.arange(count)

    def named(sizes, offset_by):
        used = int((sizes > 0).sum())
        fixed = max(1, used // 4)
        passed = fixed + (places - fixed + offset_by * (used - fixed)) % max(1, count - fixed)
        return jnp.zeros((count,), jnp.int32).at[ranking[jnp.where(places < fixed, places, passed)]].set(jnp.asarray(sizes, jnp.int32))

    sizes = jnp.where(number % 4 == 0, named(crowded, number // 4), named(common, number - number // 4 - 1))
    mixed = jax.random.permutation(jax.random.fold_in(own, 3), count)
    giver, receiver = mixed[0:count // 2 * 2:2], mixed[1:count // 2 * 2:2]
    margin = jnp.minimum(sizes[giver] - 1, most - sizes[receiver]) // 2
    margin = jnp.where((giver == ranking[0]) | (receiver == ranking[0]) | (sizes[receiver] == 0), 0, jnp.maximum(margin, 0))
    passed = jax.random.randint(jax.random.fold_in(own, 4), (count // 2,), 0, 1 << 20) % (margin + 1)
    sizes = sizes.at[giver].add(-passed).at[receiver].add(passed)
    members = jnp.searchsorted(jnp.cumsum(sizes), jnp.arange(rows * top), side="right").astype(jnp.int32)
    grid = members.reshape(top, rows).T
    grid = grid[jax.random.permutation(jax.random.fold_in(own, 1), rows)]
    offset_by = jax.random.randint(jax.random.fold_in(own, 2), (rows, 1), 0, top)
    return jnp.take_along_axis(grid, (jnp.arange(top)[None, :] + offset_by) % top, axis=1)


def portions_of(number_of, total, limit, slope, full):
    weights = [(1 << 20) // math.isqrt(rank ** slope) + 1 for rank in range(1, number_of + 1)]
    largest = limit if full else min(limit, max(-(-total // number_of), total * weights[0] // sum(weights)))
    least = 1 if total - largest >= number_of - 1 else 0
    given, rest = [largest] + [least] * (number_of - 1), total - largest - least * (number_of - 1)
    while rest > 0:
        candidates = [i for i in range(1, number_of) if given[i] < largest] or [i for i in range(1, number_of) if given[i] < limit]
        whole, budget = sum([weights[i] for i in candidates]), rest
        for i in candidates:
            addition = min(limit - given[i], max(1, budget * weights[i] // whole), rest)
            given[i] = given[i] + addition
            rest = rest - addition
    return np.array(given)


def gaussian(key, dims, scale, limit, shards=(), dtype=jnp.bfloat16):
    result = scale * jax.random.normal(key, dims, jnp.float32)
    if shards:
        result = result * shard_levels(key, dims, shards, -0.22, 0.18)
    return jnp.clip(result, -limit, limit).astype(dtype)


def setup_inputs(seed: int = 0) -> dict:
    arg_keys = jax.random.split(jax.random.key(seed), 24)
    tokens = gaussian(arg_keys[0], (BATCH, MODEL), 1.0, 6.0, ((0, 16),))
    norm_gain = jnp.clip(1.0 + 0.18 * jax.random.normal(arg_keys[1], (MODEL,), jnp.float32), 0.1, 1.9)
    query_weight = gaussian(arg_keys[2], (MODEL, HEADS * HEAD_SIZE), MODEL ** -0.5, 0.125, ((0, 16), (1, 2)))
    key_weight = gaussian(arg_keys[3], (MODEL, HEADS * HEAD_SIZE), MODEL ** -0.5, 0.125, ((0, 16), (1, 2)))
    value_weight = gaussian(arg_keys[4], (MODEL, HEADS * HEAD_SIZE), MODEL ** -0.5, 0.125, ((0, 16), (1, 2)))
    outgate_weight = gaussian(arg_keys[5], (MODEL, HEADS * HEAD_SIZE), MODEL ** -0.5, 0.125, ((0, 16), (1, 2)))
    input_weight = gaussian(arg_keys[6], (MODEL, HEADS), MODEL ** -0.5, 0.125, ((0, 16), (1, 2)))
    forget_weight = gaussian(arg_keys[7], (MODEL, HEADS), MODEL ** -0.5, 0.125, ((0, 16), (1, 2)))
    forget_bias = jnp.clip(-1.0 + 6.0 * jax.random.uniform(arg_keys[8], (HEADS,), jnp.float32) ** shard_levels(arg_keys[8], (HEADS,), ((0, 2),), -0.2, 0.2), -1.0, 5.0)
    memory = gaussian(arg_keys[9], (BATCH, HEADS, HEAD_SIZE, HEAD_SIZE), 0.3, 2.4, ((0, 16), (1, 2)), jnp.float32)
    stabilizer = jnp.clip(jax.random.uniform(arg_keys[10], (BATCH, HEADS), jnp.float32, -3.0, 3.0) * shard_levels(arg_keys[10], (BATCH, HEADS), ((0, 16), (1, 2)), -0.4, 0.0), -3.0, 3.0)
    head_gain = jnp.clip(1.0 + 0.18 * jax.random.normal(arg_keys[11], (HEADS * HEAD_SIZE,), jnp.float32), 0.1, 1.9)
    mix_weight = gaussian(arg_keys[12], (HEADS * HEAD_SIZE, MODEL), (HEADS * HEAD_SIZE) ** -0.5, 0.1875, ((0, 2), (1, 16)))
    second_gain = jnp.clip(1.0 + 0.18 * jax.random.normal(arg_keys[13], (MODEL,), jnp.float32), 0.1, 1.9)
    route_experts_keys = jax.random.split(jax.random.fold_in(arg_keys[14], 1), BATCH // SEQ_GROUP)
    route_experts_turns = jax.random.permutation(jax.random.fold_in(arg_keys[14], 3), BATCH // SEQ_GROUP)
    route_experts = jax.vmap(lambda own, number: routed_block(jax.random.fold_in(arg_keys[14], 2), own, number, SEQ_GROUP, EXPERTS, TOPK, CAPACITY, 2))(route_experts_keys, route_experts_turns).reshape((BATCH, TOPK))
    route_weight = jnp.clip(jnp.exp(math.log(1.0) - 2.3025851 * jax.random.uniform(arg_keys[15], (BATCH, TOPK), jnp.float32) ** shard_levels(arg_keys[15], (BATCH, TOPK), ((0, 16),), -0.2, 0.2)), 0.1, 1.0)
    expert_gate = gaussian(arg_keys[16], (EXPERTS, MODEL, HIDDEN_SIZE), (MODEL // 16) ** -0.5, 0.5, ((0, 16), (2, 2)))
    expert_up = gaussian(arg_keys[17], (EXPERTS, MODEL, HIDDEN_SIZE), (MODEL // 16) ** -0.5, 0.5, ((0, 16), (2, 2)))
    expert_down = gaussian(arg_keys[18], (EXPERTS, HIDDEN_SIZE, MODEL), (16 * HIDDEN_SIZE) ** -0.5, 0.03125, ((0, 16), (1, 2)))
    dense_gate = gaussian(arg_keys[19], (DENSE, MODEL), MODEL ** -0.5, 0.125, ((0, 32),))
    dense_up = gaussian(arg_keys[20], (DENSE, MODEL), MODEL ** -0.5, 0.125, ((0, 32),))
    dense_down = gaussian(arg_keys[21], (DENSE, MODEL), DENSE ** -0.5, 0.09375, ((0, 32),))
    branch_scale = jnp.clip(jax.random.uniform(arg_keys[22], (MODEL,), jnp.float32, 0.3, 1.5), 0.3, 1.5)
    return dict(tokens=tokens, norm_gain=norm_gain, query_weight=query_weight, key_weight=key_weight, value_weight=value_weight, outgate_weight=outgate_weight, input_weight=input_weight, forget_weight=forget_weight, forget_bias=forget_bias, memory=memory, stabilizer=stabilizer, head_gain=head_gain, mix_weight=mix_weight, second_gain=second_gain, route_experts=route_experts, route_weight=route_weight, expert_gate=expert_gate, expert_up=expert_up, expert_down=expert_down, dense_gate=dense_gate, dense_up=dense_up, dense_down=dense_down, branch_scale=branch_scale)


norm_eps = 1e-05
clamp_limit = 7.0
sigmoid_slope = 1.702

def rms_scale(values, gain):
    mean_square = lax.optimization_barrier(jnp.mean(values * values, axis=-1, keepdims=True))
    return values * lax.rsqrt(mean_square + norm_eps) * gain

def round_half(values):
    return lax.optimization_barrier(values.astype(jnp.bfloat16)).astype(jnp.float32)

def clamped_unit(gate_pre, up_pre):
    gate_clamped = jnp.minimum(gate_pre, clamp_limit)
    up_clamped = jnp.clip(up_pre, -clamp_limit, clamp_limit)
    return ((up_clamped + 1.0) * gate_clamped * jax.nn.sigmoid(sigmoid_slope * gate_clamped)).astype(jnp.bfloat16)

def memory_step(projected, forget_bias, memory, stabilizer, head_gain):
    query_rows, key_rows, value_rows, outgate_rows, input_pre, forget_pre = projected
    sequences, head_count = stabilizer.shape
    head_size = memory.shape[-1]
    log_forget = jax.nn.log_sigmoid(forget_pre + forget_bias)
    stab_new = jnp.maximum(log_forget + stabilizer, input_pre)
    carried = jnp.exp(log_forget + stabilizer - stab_new)
    written = jnp.exp(input_pre - stab_new)
    query_heads = query_rows.astype(jnp.float32).reshape(sequences, head_count, head_size)
    key_heads = key_rows.astype(jnp.float32).reshape(sequences, head_count, head_size) * head_size ** (-0.5)
    value_heads = value_rows.astype(jnp.float32).reshape(sequences, head_count, head_size)
    memory_new = carried[:, :, None, None] * memory + written[:, :, None, None] * value_heads[:, :, :, None] * key_heads[:, :, None, :]
    readout = jnp.einsum('bhvk,bhk->bhv', memory_new, query_heads, precision=lax.Precision.HIGHEST)
    out_gate = jax.nn.sigmoid(outgate_rows.astype(jnp.float32).reshape(sequences, head_count, head_size))
    gated = (rms_scale(readout, head_gain.reshape(head_count, head_size)) * out_gate).astype(jnp.bfloat16)
    return (gated.reshape(sequences, head_count * head_size), memory_new, stab_new)

def expert_mix(normed_second, route_experts, route_weight, expert_gate, expert_up, expert_down):
    batch_rows, model_width = normed_second.shape
    expert_count = expert_gate.shape[0]
    hidden_units = expert_gate.shape[2]
    group_units = hidden_units // N_TP
    blocks = normed_second.astype(jnp.float32).reshape(N_EP, batch_rows // N_EP, model_width)
    slots = jnp.arange(CAPACITY).astype(jnp.float32)

    def one_expert(total, index):
        matched = route_experts == index
        hit_mask = jnp.any(matched, axis=1).astype(jnp.float32).reshape(N_EP, -1)
        weights = lax.optimization_barrier(jnp.sum(jnp.where(matched, route_weight, 0.0), axis=1)).reshape(N_EP, -1)
        ranks = jnp.cumsum(hit_mask, axis=1) - 1.0
        select = hit_mask[:, None, :] * (ranks[:, None, :] == slots[None, :, None]).astype(jnp.float32)
        rows = jnp.einsum('jcs,jsd->jcd', select, blocks, precision=lax.Precision.HIGHEST)
        rows = rows.astype(jnp.bfloat16).reshape(-1, model_width)
        gate_pre = jnp.dot(rows, expert_gate[index], preferred_element_type=jnp.float32)
        up_pre = jnp.dot(rows, expert_up[index], preferred_element_type=jnp.float32)
        activity = clamped_unit(gate_pre, up_pre)
        down_weight = expert_down[index]
        outputs = jnp.zeros((rows.shape[0], model_width), jnp.float32)
        for group in range(N_TP):
            lower = group * group_units
            outputs = outputs + round_half(jnp.dot(activity[:, lower:lower + group_units], down_weight[lower:lower + group_units], preferred_element_type=jnp.float32))
        outputs = outputs.reshape(N_EP, CAPACITY, model_width)
        spread = jnp.einsum('jcs,jcd->jsd', select * weights[:, None, :], outputs, precision=lax.Precision.HIGHEST)
        return (total + spread.reshape(batch_rows, model_width), None)
    total, unused = lax.scan(one_expert, jnp.zeros((batch_rows, model_width), jnp.float32), jnp.arange(expert_count).astype(jnp.int32))
    return total

def reference(tokens, norm_gain, query_weight, key_weight, value_weight, outgate_weight, input_weight, forget_weight, forget_bias, memory, stabilizer, head_gain, mix_weight, second_gain, route_experts, route_weight, expert_gate, expert_up, expert_down, dense_gate, dense_up, dense_down, branch_scale):
    inputs_float = tokens.astype(jnp.float32)
    normed = rms_scale(inputs_float, norm_gain).astype(jnp.bfloat16)
    projected = (jnp.dot(normed, query_weight, preferred_element_type=jnp.float32).astype(jnp.bfloat16), jnp.dot(normed, key_weight, preferred_element_type=jnp.float32).astype(jnp.bfloat16), jnp.dot(normed, value_weight, preferred_element_type=jnp.float32).astype(jnp.bfloat16), jnp.dot(normed, outgate_weight, preferred_element_type=jnp.float32).astype(jnp.bfloat16), jnp.dot(normed, input_weight, preferred_element_type=jnp.float32), jnp.dot(normed, forget_weight, preferred_element_type=jnp.float32))
    gated, memory_new, stab_new = memory_step(projected, forget_bias, memory, stabilizer, head_gain)
    group_width = gated.shape[1] // N_TP
    attended = jnp.zeros_like(inputs_float)
    for group in range(N_TP):
        lower = group * group_width
        attended = attended + round_half(jnp.dot(gated[:, lower:lower + group_width], mix_weight[lower:lower + group_width], preferred_element_type=jnp.float32))
    residual = (inputs_float + attended).astype(jnp.bfloat16)
    residual_float = residual.astype(jnp.float32)
    normed_second = rms_scale(residual_float, second_gain).astype(jnp.bfloat16)
    routed = expert_mix(normed_second, route_experts, route_weight, expert_gate, expert_up, expert_down)
    dense_pre = jnp.dot(normed_second, dense_gate.T, preferred_element_type=jnp.float32)
    dense_lift = jnp.dot(normed_second, dense_up.T, preferred_element_type=jnp.float32)
    dense_act = (jax.nn.silu(dense_pre) * dense_lift).astype(jnp.bfloat16)
    dense_out = jnp.dot(dense_act, dense_down, preferred_element_type=jnp.float32)
    mixed = (residual_float + routed + branch_scale * dense_out).astype(jnp.bfloat16)
    return (mixed, memory_new, stab_new)
```

```python
import functools

import jax
import jax.numpy as jnp
from jax import lax
from jax.experimental import pallas as pl
from jax.experimental.pallas import tpu as pltpu
from jax.sharding import PartitionSpec as P

norm_eps = 1e-05
clamp_limit = 7.0
sigmoid_slope = 1.702


def rms_scale(values, gain):
    mean_square = jnp.mean(values * values, axis=-1, keepdims=True)
    return values * lax.rsqrt(mean_square + norm_eps) * gain


def clamped_unit(gate_pre, up_pre):
    gate_clamped = jnp.minimum(gate_pre, clamp_limit)
    up_clamped = jnp.clip(up_pre, -clamp_limit, clamp_limit)
    return (
        (up_clamped + 1.0) * gate_clamped * jax.nn.sigmoid(sigmoid_slope * gate_clamped)
    ).astype(jnp.bfloat16)


def memory_step(projected, forget_bias, memory, stabilizer, head_gain):
    query_rows, key_rows, value_rows, outgate_rows, input_pre, forget_pre = projected
    sequences, head_count = stabilizer.shape
    head_size = memory.shape[-1]
    log_forget = jax.nn.log_sigmoid(forget_pre + forget_bias)
    stab_new = jnp.maximum(log_forget + stabilizer, input_pre)
    carried = jnp.exp(log_forget + stabilizer - stab_new)
    written = jnp.exp(input_pre - stab_new)
    query_heads = query_rows.astype(jnp.float32).reshape(sequences, head_count, head_size)
    key_heads = key_rows.astype(jnp.float32).reshape(
        sequences, head_count, head_size
    ) * head_size ** (-0.5)
    value_heads = value_rows.astype(jnp.float32).reshape(sequences, head_count, head_size)
    memory_new = (
        carried[:, :, None, None] * memory
        + written[:, :, None, None] * value_heads[:, :, :, None] * key_heads[:, :, None, :]
    )
    readout = jnp.einsum("bhvk,bhk->bhv", memory_new, query_heads, precision=lax.Precision.HIGHEST)
    out_gate = jax.nn.sigmoid(
        outgate_rows.astype(jnp.float32).reshape(sequences, head_count, head_size)
    )
    gated = (rms_scale(readout, head_gain.reshape(head_count, head_size)) * out_gate).astype(
        jnp.bfloat16
    )
    return (gated.reshape(sequences, head_count * head_size), memory_new, stab_new)


def meet(count, me):
    barrier = pltpu.get_barrier_semaphore()

    def greet(step, carry):
        pl.semaphore_signal(
            barrier,
            inc=1,
            device_id={"ep": lax.rem(me + step, count)},
            device_id_type=pl.DeviceIdType.MESH,
        )
        return carry

    lax.fori_loop(1, count, greet, 0)
    pl.semaphore_wait(barrier, count - 1)


def link(count, me, step, source, landing, send_sem, recv_sem, gather):
    peer = lax.rem(me + step, count)
    return pltpu.make_async_remote_copy(
        src_ref=source if gather else source.at[peer],
        dst_ref=landing.at[me],
        send_sem=send_sem.at[step],
        recv_sem=recv_sem.at[step],
        device_id={"ep": peer},
        device_id_type=pl.DeviceIdType.MESH,
    )


def exchange_kernel(count, gather, source, landing, send_sem, recv_sem):
    me = lax.axis_index("ep")
    meet(count, me)

    def start(step, carry):
        link(count, me, step, source, landing, send_sem, recv_sem, gather).start()
        return carry

    def finish(step, carry):
        link(count, me, step, source, landing, send_sem, recv_sem, gather).wait()
        return carry

    lax.fori_loop(1, count, start, 0)
    landing[me] = source[...] if gather else source[me]
    lax.fori_loop(1, count, finish, 0)


def sum_kernel(count, source, total, landing, send_sem, recv_sem):
    me = lax.axis_index("ep")
    meet(count, me)

    def start(step, carry):
        link(count, me, step, source, landing, send_sem, recv_sem, False).start()
        return carry

    def finish(step, carry):
        link(count, me, step, source, landing, send_sem, recv_sem, False).wait()
        total[...] += landing[lax.rem(me + count - step, count)].astype(jnp.float32)
        return carry

    lax.fori_loop(1, count, start, 0)
    total[...] = source[me].astype(jnp.float32)
    lax.fori_loop(1, count, finish, 0)


def semaphores(count):
    return [pltpu.SemaphoreType.DMA((count,)), pltpu.SemaphoreType.DMA((count,))]


def in_vmem():
    return pl.BlockSpec(memory_space=pltpu.VMEM)


def exchange(blocks, count, name, gather=False):
    shape = (count,) + blocks.shape if gather else blocks.shape
    return pl.pallas_call(
        functools.partial(exchange_kernel, count, gather),
        out_shape=jax.ShapeDtypeStruct(shape, blocks.dtype),
        in_specs=[in_vmem()],
        out_specs=in_vmem(),
        scratch_shapes=semaphores(count),
        compiler_params=pltpu.CompilerParams(
            collective_id=name, has_side_effects=True, vmem_limit_bytes=16 * 2**20
        ),
    )(blocks)


def exchange_sum(blocks, count, name):
    return pl.pallas_call(
        functools.partial(sum_kernel, count),
        out_shape=jax.ShapeDtypeStruct(blocks.shape[1:], jnp.float32),
        in_specs=[in_vmem()],
        out_specs=in_vmem(),
        scratch_shapes=[pltpu.VMEM(blocks.shape, blocks.dtype)] + semaphores(count),
        compiler_params=pltpu.CompilerParams(
            collective_id=name, has_side_effects=True, vmem_limit_bytes=24 * 2**20
        ),
    )(blocks)


def split_parts(values, number):
    parts = []
    for _ in range(number):
        part = lax.reduce_precision(values, 8, 7)
        parts.append(part.astype(jnp.bfloat16))
        values = values - part
    return parts


def body(
    tokens,
    norm_gain,
    query_weight,
    key_weight,
    value_weight,
    outgate_weight,
    input_weight,
    forget_weight,
    forget_bias,
    memory,
    stabilizer,
    head_gain,
    mix_weight,
    second_gain,
    route_experts,
    route_weight,
    expert_gate,
    expert_up,
    expert_down,
    dense_gate,
    dense_up,
    dense_down,
    branch_scale,
):
    sequences, model_width = tokens.shape
    ep_count = lax.axis_size("ep")
    tp_count = lax.axis_size("tp")
    me, side = lax.axis_index("ep"), lax.axis_index("tp")
    swap = [(i, tp_count - 1 - i) for i in range(tp_count)]
    rows = sequences * ep_count
    part_width = model_width // tp_count
    own_width = model_width // ep_count
    lanes = 128
    first = side == 0

    inputs_float = tokens.astype(jnp.float32)
    normed = rms_scale(inputs_float, norm_gain).astype(jnp.bfloat16)
    matched = route_experts[:, :, None] == jnp.arange(ep_count)[None, None, :]
    weights = jnp.sum(jnp.where(matched, route_weight[:, :, None], 0.0), axis=1)
    weight_parts = jnp.stack(split_parts(weights, 3), axis=-1)
    weight_parts = jnp.pad(weight_parts, ((0, 0), (0, 0), (0, lanes - 3)))
    payload = jnp.concatenate(
        [
            normed.reshape(sequences, ep_count, own_width),
            tokens.reshape(sequences, ep_count, own_width),
            weight_parts,
        ],
        axis=2,
    ).transpose(1, 0, 2)
    columns = exchange(payload, ep_count, 1).reshape(rows, -1)
    token_columns = columns[:, own_width : 2 * own_width]
    row_weight = jnp.sum(
        columns[:, 2 * own_width : 2 * own_width + 3].astype(jnp.float32), axis=1, keepdims=True
    )

    wide = jnp.concatenate((query_weight, key_weight, value_weight, outgate_weight), axis=1)
    thin = jnp.concatenate((input_weight, forget_weight), axis=1)
    own_columns = columns[:, :own_width]
    wide_sums = jnp.dot(own_columns, wide, preferred_element_type=jnp.float32)
    thin_sums = jnp.dot(own_columns, thin, preferred_element_type=jnp.float32)
    gates = thin.shape[1]
    upper, under = split_parts(thin_sums, 2)
    partials = jnp.concatenate(
        [
            wide_sums.astype(jnp.bfloat16),
            jnp.pad(jnp.concatenate([upper, under], axis=1), ((0, 0), (0, lanes - 2 * gates))),
        ],
        axis=1,
    )
    sums = exchange_sum(partials.reshape(ep_count, sequences, -1), ep_count, 2)
    width = query_weight.shape[1]
    gate_sums = sums[:, 4 * width : 4 * width + gates] + sums[:, 4 * width + gates : 4 * width + 2 * gates]
    projected = tuple(
        sums[:, i * width : (i + 1) * width].astype(jnp.bfloat16) for i in range(4)
    ) + (gate_sums[:, : gates // 2], gate_sums[:, gates // 2 :])
    gated, memory_new, stab_new = memory_step(projected, forget_bias, memory, stabilizer, head_gain)

    all_gated = exchange(gated, ep_count, 3, gather=True).reshape(rows, -1)
    partial_value = jnp.dot(
        all_gated, mix_weight, preferred_element_type=jnp.float32
    ).astype(jnp.bfloat16)
    half = rows // tp_count
    upper, under = partial_value[:half], partial_value[half:]
    kept = jnp.where(first, upper, under)
    came = lax.ppermute(jnp.where(first, under, upper), "tp", swap)
    attended = kept.astype(jnp.float32) + came.astype(jnp.float32)
    token_half = jnp.where(first, token_columns[:half], token_columns[half:])
    residual_part = (token_half.astype(jnp.float32) + attended).astype(jnp.bfloat16)
    half_rows = exchange(residual_part, ep_count, 4, gather=True)
    half_rows = half_rows.transpose(1, 0, 2).reshape(half, model_width)
    other_rows = lax.ppermute(half_rows, "tp", swap)
    residual = jnp.concatenate(
        [jnp.where(first, half_rows, other_rows), jnp.where(first, other_rows, half_rows)], axis=0
    )
    normed_second = rms_scale(residual.astype(jnp.float32), second_gain).astype(jnp.bfloat16)

    gate_pre = jnp.dot(normed_second, expert_gate[0], preferred_element_type=jnp.float32)
    up_pre = jnp.dot(normed_second, expert_up[0], preferred_element_type=jnp.float32)
    expert_act = clamped_unit(gate_pre, up_pre)
    expert_out = jnp.dot(expert_act, expert_down[0], preferred_element_type=jnp.float32)
    gate_rows = jnp.einsum(
        "td,fd->tf", normed_second, dense_gate, preferred_element_type=jnp.float32
    )
    lift_rows = jnp.einsum("td,fd->tf", normed_second, dense_up, preferred_element_type=jnp.float32)
    dense_act = (jax.nn.silu(gate_rows) * lift_rows).astype(jnp.bfloat16)
    dense_out = jnp.dot(dense_act, dense_down, preferred_element_type=jnp.float32)
    term = dense_out * branch_scale + row_weight * expert_out
    left, right = term[:, :part_width], term[:, part_width:]
    passed = jnp.where(first, right, left).astype(jnp.bfloat16)
    received = lax.ppermute(passed, "tp", swap).astype(jnp.float32)
    summed = (jnp.where(first, left, right) + received).astype(jnp.bfloat16)
    branches = exchange_sum(summed.reshape(ep_count, sequences, part_width), ep_count, 5)
    own_residual = lax.dynamic_slice(
        residual, (me * sequences, side * part_width), (sequences, part_width)
    )
    mixed = own_residual.astype(jnp.float32) + branches
    return (mixed.astype(jnp.bfloat16), memory_new, stab_new)


def solution(mesh):
    in_specs = (
        P("ep", None),
        P(),
        P("ep", "tp"),
        P("ep", "tp"),
        P("ep", "tp"),
        P("ep", "tp"),
        P("ep", "tp"),
        P("ep", "tp"),
        P("tp"),
        P("ep", "tp", None, None),
        P("ep", "tp"),
        P("tp"),
        P("tp", "ep"),
        P(),
        P("ep", None),
        P("ep", None),
        P("ep", None, "tp"),
        P("ep", None, "tp"),
        P("ep", "tp", None),
        P(("ep", "tp"), None),
        P(("ep", "tp"), None),
        P(("ep", "tp"), None),
        P(),
    )
    out_specs = (P("ep", "tp"), P("ep", "tp", None, None), P("ep", "tp"))
    return jax.shard_map(body, mesh=mesh, in_specs=in_specs, out_specs=out_specs, check_vma=False)
```

```python
import functools

import jax
import jax.numpy as jnp
from jax import lax
from jax.experimental import pallas as pl
from jax.experimental.pallas import tpu as pltpu
from jax.sharding import PartitionSpec as P

norm_eps = 1e-05
clamp_limit = 7.0
sigmoid_slope = 1.702


def rms_scale(values, gain):
    mean_square = jnp.mean(values * values, axis=-1, keepdims=True)
    return values * lax.rsqrt(mean_square + norm_eps) * gain


def clamped_unit(gate_pre, up_pre):
    gate_clamped = jnp.minimum(gate_pre, clamp_limit)
    up_clamped = jnp.clip(up_pre, -clamp_limit, clamp_limit)
    return (
        (up_clamped + 1.0) * gate_clamped * jax.nn.sigmoid(sigmoid_slope * gate_clamped)
    ).astype(jnp.bfloat16)


def memory_step(projected, forget_bias, memory, stabilizer, head_gain):
    query_rows, key_rows, value_rows, outgate_rows, input_pre, forget_pre = projected
    sequences, head_count = stabilizer.shape
    head_size = memory.shape[-1]
    log_forget = jax.nn.log_sigmoid(forget_pre + forget_bias)
    stab_new = jnp.maximum(log_forget + stabilizer, input_pre)
    carried = jnp.exp(log_forget + stabilizer - stab_new)
    written = jnp.exp(input_pre - stab_new)
    query_heads = query_rows.astype(jnp.float32).reshape(sequences, head_count, head_size)
    key_heads = key_rows.astype(jnp.float32).reshape(
        sequences, head_count, head_size
    ) * head_size ** (-0.5)
    value_heads = value_rows.astype(jnp.float32).reshape(sequences, head_count, head_size)
    memory_new = (
        carried[:, :, None, None] * memory
        + written[:, :, None, None] * value_heads[:, :, :, None] * key_heads[:, :, None, :]
    )
    readout = jnp.einsum("bhvk,bhk->bhv", memory_new, query_heads, precision=lax.Precision.HIGHEST)
    out_gate = jax.nn.sigmoid(
        outgate_rows.astype(jnp.float32).reshape(sequences, head_count, head_size)
    )
    gated = (rms_scale(readout, head_gain.reshape(head_count, head_size)) * out_gate).astype(
        jnp.bfloat16
    )
    return (gated.reshape(sequences, head_count * head_size), memory_new, stab_new)


def meet(count, me):
    barrier = pltpu.get_barrier_semaphore()

    def greet(step, carry):
        pl.semaphore_signal(
            barrier,
            inc=1,
            device_id={"ep": lax.rem(me + step, count)},
            device_id_type=pl.DeviceIdType.MESH,
        )
        return carry

    lax.fori_loop(1, count, greet, 0)
    pl.semaphore_wait(barrier, count - 1)


def link(count, me, step, source, landing, send_sem, recv_sem, gather):
    peer = lax.rem(me + step, count)
    return pltpu.make_async_remote_copy(
        src_ref=source if gather else source.at[peer],
        dst_ref=landing.at[me],
        send_sem=send_sem.at[step],
        recv_sem=recv_sem.at[step],
        device_id={"ep": peer},
        device_id_type=pl.DeviceIdType.MESH,
    )


def sum_kernel(count, source, total, landing, send_sem, recv_sem):
    me = lax.axis_index("ep")
    meet(count, me)

    def start(step, carry):
        link(count, me, step, source, landing, send_sem, recv_sem, False).start()
        return carry

    def finish(step, carry):
        link(count, me, step, source, landing, send_sem, recv_sem, False).wait()
        total[...] += landing[lax.rem(me + count - step, count)].astype(jnp.float32)
        return carry

    lax.fori_loop(1, count, start, 0)
    total[...] = source[me].astype(jnp.float32)
    lax.fori_loop(1, count, finish, 0)


def semaphores(count):
    return [pltpu.SemaphoreType.DMA((count,)), pltpu.SemaphoreType.DMA((count,))]


def in_vmem():
    return pl.BlockSpec(memory_space=pltpu.VMEM)


def exchange_sum(blocks, count, name):
    return pl.pallas_call(
        functools.partial(sum_kernel, count),
        out_shape=jax.ShapeDtypeStruct(blocks.shape[1:], jnp.float32),
        in_specs=[in_vmem()],
        out_specs=in_vmem(),
        scratch_shapes=[pltpu.VMEM(blocks.shape, blocks.dtype)] + semaphores(count),
        compiler_params=pltpu.CompilerParams(
            collective_id=name, has_side_effects=True, vmem_limit_bytes=24 * 2**20
        ),
    )(blocks)


def project_kernel(
    count, gates, payload, query, key, value, outgate, thin, landing, total,
    partial, arriving, send_one, recv_one, send_two, recv_two,
):
    me = lax.axis_index("ep")
    depth = query.shape[0]
    width = query.shape[1]
    sequences = payload.shape[1]
    meet(count, me)

    def start(step, carry):
        link(count, me, step, payload, landing, send_one, recv_one, False).start()
        return carry

    def finish(step, carry):
        link(count, me, step, payload, landing, send_one, recv_one, False).wait()
        return carry

    lax.fori_loop(1, count, start, 0)
    landing[me] = payload[me]
    lax.fori_loop(1, count, finish, 0)
    rows = landing[:, :, :depth].reshape(count * sequences, depth)
    small = jnp.dot(rows, thin[...], preferred_element_type=jnp.float32)
    upper = small.astype(jnp.bfloat16).astype(jnp.float32)
    place = lax.broadcasted_iota(jnp.int32, small.shape, 1)
    small = jnp.where(place < gates, upper, small - upper).astype(jnp.bfloat16)
    partial[:, :, 4 * width :] = small.reshape(count, sequences, small.shape[1])
    for number, weight in enumerate((query, key, value, outgate)):
        sums = jnp.dot(rows, weight[...], preferred_element_type=jnp.float32)
        partial[:, :, number * width : (number + 1) * width] = sums.astype(jnp.bfloat16).reshape(
            count, sequences, width
        )

    def start_sum(step, carry):
        link(count, me, step, partial, arriving, send_two, recv_two, False).start()
        return carry

    def finish_sum(step, carry):
        link(count, me, step, partial, arriving, send_two, recv_two, False).wait()
        total[...] += arriving[lax.rem(me + count - step, count)].astype(jnp.float32)
        return carry

    lax.fori_loop(1, count, start_sum, 0)
    total[...] = partial[me].astype(jnp.float32)
    lax.fori_loop(1, count, finish_sum, 0)


def project(payload, weights, thin, count, gates, name):
    sequences = payload.shape[1]
    width = 4 * weights[0].shape[1] + thin.shape[1]
    block = (count, sequences, width)
    return pl.pallas_call(
        functools.partial(project_kernel, count, gates),
        out_shape=(
            jax.ShapeDtypeStruct(payload.shape, payload.dtype),
            jax.ShapeDtypeStruct((sequences, width), jnp.float32),
        ),
        in_specs=[in_vmem()] * 6,
        out_specs=(in_vmem(), in_vmem()),
        scratch_shapes=[pltpu.VMEM(block, jnp.bfloat16)] * 2 + semaphores(count) + semaphores(count),
        compiler_params=pltpu.CompilerParams(
            collective_id=name, has_side_effects=True, vmem_limit_bytes=32 * 2**20
        ),
    )(payload, *weights, thin)


def across(side, source, landing, send_sem, recv_sem):
    return pltpu.make_async_remote_copy(
        src_ref=source,
        dst_ref=landing,
        send_sem=send_sem,
        recv_sem=recv_sem,
        device_id={"tp": 1 - side},
        device_id_type=pl.DeviceIdType.MESH,
    )


def mix_kernel(
    count, gated, mix, tokens, gathered, landing, partial, came, mine,
    send_one, recv_one, send_two, recv_two, send_three, recv_three, send_four, recv_four,
):
    me, side = lax.axis_index("ep"), lax.axis_index("tp")
    barrier = pltpu.get_barrier_semaphore()

    def greet(step, carry):
        pl.semaphore_signal(
            barrier,
            inc=1,
            device_id={"ep": lax.rem(me + step, count)},
            device_id_type=pl.DeviceIdType.MESH,
        )
        return carry

    lax.fori_loop(1, count, greet, 0)
    pl.semaphore_signal(
        barrier, inc=1, device_id={"tp": 1 - side}, device_id_type=pl.DeviceIdType.MESH
    )
    pl.semaphore_wait(barrier, count)

    def start(step, carry):
        link(count, me, step, gated, landing, send_one, recv_one, True).start()
        return carry

    def finish(step, carry):
        link(count, me, step, gated, landing, send_one, recv_one, True).wait()
        return carry

    lax.fori_loop(1, count, start, 0)
    landing[me] = gated[...]
    lax.fori_loop(1, count, finish, 0)
    rows = landing[...].reshape(-1, gated.shape[1])
    sums = jnp.dot(rows, mix[...], preferred_element_type=jnp.float32)
    partial[...] = sums.astype(jnp.bfloat16).reshape(partial.shape)
    swap = across(side, partial.at[1 - side], came, send_two, recv_two)
    swap.start()
    swap.wait()
    attended = partial[side].astype(jnp.float32) + came[...].astype(jnp.float32)
    residual = (tokens[side].astype(jnp.float32) + attended).astype(jnp.bfloat16)
    mine[...] = residual
    own = gathered.at[side]

    def start_rows(step, carry):
        link(count, me, step, mine, own, send_three, recv_three, True).start()
        return carry

    def relay(step, carry):
        link(count, me, step, mine, own, send_three, recv_three, True).wait()
        origin = lax.rem(me + count - step, count)
        place = gathered.at[side, origin]
        across(side, place, place, send_four.at[step], recv_four.at[step]).start()
        return carry

    def finish_rows(step, carry):
        place = gathered.at[side, me]
        across(side, place, place, send_four.at[step], recv_four.at[step]).wait()
        return carry

    lax.fori_loop(1, count, start_rows, 0)
    across(side, mine, gathered.at[side, me], send_four.at[0], recv_four.at[0]).start()
    gathered[side, me] = residual
    lax.fori_loop(1, count, relay, 0)
    lax.fori_loop(0, count, finish_rows, 0)


def mix_rows(gated, mix, tokens, count, name):
    half, own_width = tokens.shape[1:]
    block = pltpu.VMEM((half, own_width), jnp.bfloat16)
    return pl.pallas_call(
        functools.partial(mix_kernel, count),
        out_shape=jax.ShapeDtypeStruct((2, count, half, own_width), jnp.bfloat16),
        in_specs=[in_vmem()] * 3,
        out_specs=in_vmem(),
        scratch_shapes=[
            pltpu.VMEM((count,) + gated.shape, jnp.bfloat16),
            pltpu.VMEM((2, half, own_width), jnp.bfloat16),
            block,
            block,
        ]
        + semaphores(count)
        + [pltpu.SemaphoreType.DMA, pltpu.SemaphoreType.DMA]
        + semaphores(count)
        + semaphores(count),
        compiler_params=pltpu.CompilerParams(
            collective_id=name, has_side_effects=True, vmem_limit_bytes=32 * 2**20
        ),
    )(gated, mix, tokens)


def split_parts(values, number):
    parts = []
    for _ in range(number):
        part = lax.reduce_precision(values, 8, 7)
        parts.append(part.astype(jnp.bfloat16))
        values = values - part
    return parts


def body(
    tokens,
    norm_gain,
    query_weight,
    key_weight,
    value_weight,
    outgate_weight,
    input_weight,
    forget_weight,
    forget_bias,
    memory,
    stabilizer,
    head_gain,
    mix_weight,
    second_gain,
    route_experts,
    route_weight,
    expert_gate,
    expert_up,
    expert_down,
    dense_gate,
    dense_up,
    dense_down,
    branch_scale,
):
    sequences, model_width = tokens.shape
    ep_count = lax.axis_size("ep")
    tp_count = lax.axis_size("tp")
    me, side = lax.axis_index("ep"), lax.axis_index("tp")
    swap = [(i, tp_count - 1 - i) for i in range(tp_count)]
    rows = sequences * ep_count
    part_width = model_width // tp_count
    own_width = model_width // ep_count
    lanes = 128
    first = side == 0

    inputs_float = tokens.astype(jnp.float32)
    normed = rms_scale(inputs_float, norm_gain).astype(jnp.bfloat16)
    matched = route_experts[:, :, None] == jnp.arange(ep_count)[None, None, :]
    weights = jnp.sum(jnp.where(matched, route_weight[:, :, None], 0.0), axis=1)
    weight_parts = jnp.stack(split_parts(weights, 3), axis=-1)
    weight_parts = jnp.pad(weight_parts, ((0, 0), (0, 0), (0, lanes - 3)))
    payload = jnp.concatenate(
        [
            normed.reshape(sequences, ep_count, own_width),
            tokens.reshape(sequences, ep_count, own_width),
            weight_parts,
        ],
        axis=2,
    ).transpose(1, 0, 2)
    thin = jnp.concatenate((input_weight, forget_weight), axis=1)
    gates = thin.shape[1]
    thin = jnp.pad(jnp.concatenate((thin, thin), axis=1), ((0, 0), (0, lanes - 2 * gates)))
    wide = (query_weight, key_weight, value_weight, outgate_weight)
    columns, sums = project(payload, wide, thin, ep_count, gates, 1)
    columns = columns.reshape(rows, -1)
    token_columns = columns[:, own_width : 2 * own_width]
    row_weight = jnp.sum(
        columns[:, 2 * own_width : 2 * own_width + 3].astype(jnp.float32), axis=1, keepdims=True
    )
    width = query_weight.shape[1]
    gate_sums = sums[:, 4 * width : 4 * width + gates] + sums[:, 4 * width + gates : 4 * width + 2 * gates]
    projected = tuple(
        sums[:, i * width : (i + 1) * width].astype(jnp.bfloat16) for i in range(4)
    ) + (gate_sums[:, : gates // 2], gate_sums[:, gates // 2 :])
    gated, memory_new, stab_new = memory_step(projected, forget_bias, memory, stabilizer, head_gain)

    token_halves = token_columns.reshape(tp_count, rows // tp_count, own_width)
    gathered = mix_rows(gated, mix_weight, token_halves, ep_count, 2)
    residual = gathered.transpose(0, 2, 1, 3).reshape(rows, model_width)
    normed_second = rms_scale(residual.astype(jnp.float32), second_gain).astype(jnp.bfloat16)

    gate_pre = jnp.dot(normed_second, expert_gate[0], preferred_element_type=jnp.float32)
    up_pre = jnp.dot(normed_second, expert_up[0], preferred_element_type=jnp.float32)
    expert_act = clamped_unit(gate_pre, up_pre)
    expert_out = jnp.dot(expert_act, expert_down[0], preferred_element_type=jnp.float32)
    gate_rows = jnp.einsum(
        "td,fd->tf", normed_second, dense_gate, preferred_element_type=jnp.float32
    )
    lift_rows = jnp.einsum("td,fd->tf", normed_second, dense_up, preferred_element_type=jnp.float32)
    dense_act = (jax.nn.silu(gate_rows) * lift_rows).astype(jnp.bfloat16)
    dense_out = jnp.dot(dense_act, dense_down, preferred_element_type=jnp.float32)
    term = dense_out * branch_scale + row_weight * expert_out
    left, right = term[:, :part_width], term[:, part_width:]
    passed = jnp.where(first, right, left).astype(jnp.bfloat16)
    received = lax.ppermute(passed, "tp", swap).astype(jnp.float32)
    summed = (jnp.where(first, left, right) + received).astype(jnp.bfloat16)
    branches = exchange_sum(summed.reshape(ep_count, sequences, part_width), ep_count, 5)
    own_residual = lax.dynamic_slice(
        residual, (me * sequences, side * part_width), (sequences, part_width)
    )
    mixed = own_residual.astype(jnp.float32) + branches
    return (mixed.astype(jnp.bfloat16), memory_new, stab_new)


def solution(mesh):
    in_specs = (
        P("ep", None),
        P(),
        P("ep", "tp"),
        P("ep", "tp"),
        P("ep", "tp"),
        P("ep", "tp"),
        P("ep", "tp"),
        P("ep", "tp"),
        P("tp"),
        P("ep", "tp", None, None),
        P("ep", "tp"),
        P("tp"),
        P("tp", "ep"),
        P(),
        P("ep", None),
        P("ep", None),
        P("ep", None, "tp"),
        P("ep", None, "tp"),
        P("ep", "tp", None),
        P(("ep", "tp"), None),
        P(("ep", "tp"), None),
        P(("ep", "tp"), None),
        P(),
    )
    out_specs = (P("ep", "tp"), P("ep", "tp", None, None), P("ep", "tp"))
    return jax.shard_map(body, mesh=mesh, in_specs=in_specs, out_specs=out_specs, check_vma=False)
```
